128 devices in a mesh: grp: 4 (over y, x), ep: 32 (over z, core).
Axes of the slice: x: 2, y: 2, z: 16, core: 2. Of those that a mesh axis runs over, the one named last changes fastest.
The devices are a block of a 8x8x16 slice.
Arguments:
- residual: bfloat16 [64, 4096], P('grp', 'ep'), parts along dimension 0, may hold values from -6 to 6
- head_states: float32 [256, 512, 1024], P(('grp', 'ep')), parts along dimension 0, may hold values from -6 to 6
- first_gain: bfloat16 [4096], replicated, may hold values from 0.099609375 to 1.8984375
- w_query: bfloat16 [4096, 2048], P(None, 'ep'), may hold values from -0.09375 to 0.09375
- w_key: bfloat16 [4096, 2048], P(None, 'ep'), may hold values from -0.09375 to 0.09375
- w_value: bfloat16 [4096, 4096], P(None, 'ep'), may hold values from -0.09375 to 0.09375
- w_gate: bfloat16 [4096, 4096], P(None, 'ep'), may hold values from -0.09375 to 0.09375
- w_low: bfloat16 [4096, 16], replicated, may hold values from -0.09375 to 0.09375
- w_decay: bfloat16 [16, 2048], replicated, may hold values from -15 to 15
- decay_bias: float32 [2048], replicated, may hold values from -40 to 4
- head_gain: bfloat16 [1024], replicated, may hold values from 0.099609375 to 1.8984375
- w_output: bfloat16 [4096, 4096], P(None, 'ep'), may hold values from -0.09375 to 0.09375
- second_gain: bfloat16 [4096], replicated, may hold values from 0.099609375 to 1.8984375
- routes: int32 [64, 2], P('grp'), parts along dimension 0, may hold values from 0 to 31, as said below
- group_logits: float32 [64, 4], P('grp'), parts along dimension 0, may hold values from -12 to 12
- expert_logits: float32 [64, 2], P('grp'), parts along dimension 0, may hold values from -9 to 9
- expert_gate: bfloat16 [32, 4096, 512], P('ep'), may hold values from -0.09375 to 0.09375
- expert_up: bfloat16 [32, 4096, 512], P('ep'), may hold values from -0.09375 to 0.09375
- expert_down: bfloat16 [32, 512, 4096], P('ep'), may hold values from -0.25 to 0.25
Outputs:
- layer_out: bfloat16 [64, 4096], P('grp', 'ep'), parts along dimension 0
- new_states: float32 [256, 512, 1024], P(('grp', 'ep')), parts along dimension 0
The draws below stay inside these ranges and needn't reach their ends.
There are 4 independent parts, one for each index of `grp`. The reference program is written for one: setup_inputs(seed, part) draws one part's arguments, and reference() takes and returns one part's arrays. A program takes and returns all parts, laid end to end along the dimension named above; an argument that names none is the same for every part. Nothing has to cross between parts.
Inputs may be any that keep to these rules, and one draw needn't show every extreme that they name: `routes`: each row names 2 different experts of one group (numbers g * 8 to g * 8 + 7). No expert is named by more than 2 rows, and in every draw all experts of one group are named by exactly 2 rows.
All inputs are finite; a program needn't handle non-finite values.
Results may differ from the reference program's by a relative error of at most 0.014.
Values may be sent and summed in bfloat16 or wider, within the bound.
A program may use at most 128 MiB of HBM per device.

```python
import jax
import jax.numpy as jnp
from jax import lax

D = 4096
HEADS = 4
DK = 512
DV = 1024
RANK = 16
FF = 512
GROUPS = 4
TOP = 2
SEQS = 16
PAIRS = 64
EXPERTS = 32
EPG = 8
CAP = 2


def draw_routes(key, part):
    order_key, full_key, other_key, perm_key = jax.random.split(jax.random.fold_in(key, 17), 4)
    full_count = EPG * CAP // TOP
    order = jax.random.permutation(order_key, SEQS)
    full_group = jax.random.randint(full_key, (), 0, GROUPS, dtype=jnp.int32)
    others = jax.random.randint(other_key, (SEQS,), 0, GROUPS - 1, dtype=jnp.int32)
    others = others + (others >= full_group).astype(jnp.int32)
    position = jnp.arange(SEQS, dtype=jnp.int32)
    by_position = jnp.where(position < full_count, full_group, others)
    group = jnp.zeros((SEQS,), jnp.int32).at[order].set(by_position)
    member = (group[:, None] == jnp.arange(GROUPS, dtype=jnp.int32)[None, :]).astype(jnp.int32)
    before = jnp.cumsum(member, axis=0) - member
    rank = jnp.sum(before * member, axis=1)
    tables = jax.vmap(lambda one: jax.random.permutation(one, EPG))(jax.random.split(perm_key, GROUPS)).astype(jnp.int32)
    slots = TOP * rank[:, None] + jnp.arange(TOP, dtype=jnp.int32)[None, :]
    local = slots % EPG
    chosen = tables[group[:, None], local]
    return (group[:, None] * EPG + chosen).astype(jnp.int32)


def steps_of(own_key, dims, pieces, low, largest):
    factor_of, own = 1.0, jax.random.fold_in(own_key, 6)
    for dim, parts in pieces:
        steps = jnp.exp(jax.random.uniform(jax.random.fold_in(own, dim), (parts,), jnp.float32, low / len(pieces), largest / len(pieces)))
        factor_of = factor_of * jnp.repeat(steps, dims[dim] // parts).reshape([-1 if axis == dim else 1 for axis in range(len(dims))])
    return factor_of


def gaussian(rng, extent, scale, bound, cuts=(), held_as=jnp.bfloat16):
    level = steps_of(rng, extent, cuts, -0.22, 0.18) if cuts else 1.0
    array = jax.random.normal(rng, extent, jnp.float32) * scale * level
    return jnp.minimum(jnp.maximum(array, -bound), bound).astype(held_as)


def setup_inputs(seed: int = 0, part: int = 0) -> dict:
    arg_keys = jax.random.split(jax.random.key(seed), 20)
    part_splits = jax.random.split(jax.random.fold_in(arg_keys[19], part), 20)
    return {
        "residual": gaussian(part_splits[0], (SEQS, D), 1.0, 6.0, ((1, 32),)),
        "head_states": gaussian(part_splits[1], (PAIRS, DK, DV), 1.0, 6.0, ((0, 32),), jnp.float32),
        "first_gain": jnp.clip(1.0 + 0.18 * jax.random.normal(arg_keys[2], (D,), jnp.float32), 0.099609375, 1.8984375).astype(jnp.bfloat16),
        "w_query": gaussian(arg_keys[3], (D, HEADS * DK), D ** -0.5, 0.09375, ((1, 32),)),
        "w_key": gaussian(arg_keys[4], (D, HEADS * DK), D ** -0.5, 0.09375, ((1, 32),)),
        "w_value": gaussian(arg_keys[5], (D, HEADS * DV), D ** -0.5, 0.09375, ((1, 32),)),
        "w_gate": gaussian(arg_keys[6], (D, HEADS * DV), D ** -0.5, 0.09375, ((1, 32),)),
        "w_low": gaussian(arg_keys[7], (D, RANK), D ** -0.5, 0.09375),
        "w_decay": gaussian(arg_keys[8], (RANK, HEADS * DK), 3.0, 15.0),
        "decay_bias": jnp.clip(jax.random.uniform(arg_keys[9], (HEADS * DK,), jnp.float32, -40.0, 4.0), -40.0, 4.0),
        "head_gain": jnp.clip(1.0 + 0.18 * jax.random.normal(arg_keys[10], (DV,), jnp.float32), 0.099609375, 1.8984375).astype(jnp.bfloat16),
        "w_output": gaussian(arg_keys[11], (HEADS * DV, D), (HEADS * DV) ** -0.5, 0.09375, ((1, 32),)),
        "second_gain": jnp.clip(1.0 + 0.18 * jax.random.normal(arg_keys[12], (D,), jnp.float32), 0.099609375, 1.8984375).astype(jnp.bfloat16),
        "routes": draw_routes(jax.random.fold_in(jax.random.fold_in(arg_keys[19], part), 71), part),
        "group_logits": gaussian(part_splits[14], (SEQS, GROUPS), 2.0, 12.0, (), jnp.float32),
        "expert_logits": gaussian(part_splits[15], (SEQS, TOP), 1.5, 9.0, (), jnp.float32),
        "expert_gate": gaussian(arg_keys[16], (EXPERTS, D, FF), D ** -0.5, 0.09375, ((0, 32),)),
        "expert_up": gaussian(arg_keys[17], (EXPERTS, D, FF), D ** -0.5, 0.09375, ((0, 32),)),
        "expert_down": gaussian(arg_keys[18], (EXPERTS, FF, D), FF ** -0.5, 0.25, ((0, 32),)),
    }


norm_eps = 1e-06
decay_tau = 16.0

def rms_scale(values, gain):
    floats = values.astype(jnp.float32)
    return floats * lax.rsqrt(lax.optimization_barrier(jnp.mean(floats * floats, axis=-1, keepdims=True)) + norm_eps) * gain.astype(jnp.float32)

def route_weights(routes, group_logits, expert_logits, per_group):
    group_exp = jnp.exp(group_logits)
    group_prob = group_exp / lax.optimization_barrier(jnp.sum(group_exp, axis=1, keepdims=True))
    chosen = routes[:, 0] // per_group
    groups_row = jnp.arange(group_logits.shape[1], dtype=jnp.int32)
    picked = lax.optimization_barrier(jnp.sum(group_prob * (chosen[:, None] == groups_row[None, :]).astype(jnp.float32), axis=1))
    expert_exp = jnp.exp(expert_logits)
    return expert_exp / lax.optimization_barrier(jnp.sum(expert_exp, axis=1, keepdims=True)) * picked[:, None]

def reference(residual, head_states, first_gain, w_query, w_key, w_value, w_gate, w_low, w_decay, decay_bias, head_gain, w_output, second_gain, routes, group_logits, expert_logits, expert_gate, expert_up, expert_down):
    normed = rms_scale(residual, first_gain).astype(jnp.bfloat16)
    query = jnp.dot(normed, w_query, preferred_element_type=jnp.float32).astype(jnp.bfloat16).reshape(PAIRS, DK)
    key = jnp.dot(normed, w_key, preferred_element_type=jnp.float32).astype(jnp.bfloat16).reshape(PAIRS, DK)
    value = jnp.dot(normed, w_value, preferred_element_type=jnp.float32).astype(jnp.bfloat16).reshape(PAIRS, DV)
    gate = jnp.dot(normed, w_gate, preferred_element_type=jnp.float32).astype(jnp.bfloat16).reshape(PAIRS, DV)
    low = jnp.dot(normed, w_low, preferred_element_type=jnp.float32)
    decay_pre = jnp.dot(low, w_decay.astype(jnp.float32), precision=lax.Precision.HIGHEST) + decay_bias
    log_decay = jax.nn.log_sigmoid(decay_pre.reshape(PAIRS, DK)) / decay_tau
    new_states = head_states * jnp.exp(log_decay)[:, :, None] + key.astype(jnp.float32)[:, :, None] * value.astype(jnp.float32)[:, None, :]
    read = jnp.einsum('pk,pkv->pv', query.astype(jnp.float32) * DK ** (-0.5), new_states, precision=lax.Precision.HIGHEST)
    mixed = (rms_scale(read, head_gain) * jax.nn.silu(gate.astype(jnp.float32))).astype(jnp.bfloat16)
    branch = jnp.dot(mixed.reshape(SEQS, HEADS * DV), w_output, preferred_element_type=jnp.float32).astype(jnp.bfloat16)
    stream = (residual.astype(jnp.float32) + branch.astype(jnp.float32)).astype(jnp.bfloat16)
    expert_in = rms_scale(stream, second_gain).astype(jnp.bfloat16)
    weights = route_weights(routes, group_logits, expert_logits, EPG)
    every = jnp.arange(EXPERTS, dtype=jnp.int32)
    combine = lax.optimization_barrier(jnp.sum(weights[:, :, None] * (routes[:, :, None] == every[None, None, :]).astype(jnp.float32), axis=1))

    def one_expert(total, inputs):
        gate_w, up_w, down_w, share = inputs
        gate_part = jnp.dot(expert_in, gate_w, preferred_element_type=jnp.float32)
        up_part = jnp.dot(expert_in, up_w, preferred_element_type=jnp.float32)
        active = (jax.nn.silu(gate_part) * up_part * share[:, None]).astype(jnp.bfloat16)
        contribution = jnp.dot(active, down_w, preferred_element_type=jnp.float32).astype(jnp.bfloat16)
        return (total + contribution.astype(jnp.float32), None)
    start = jnp.zeros((SEQS, D), jnp.float32)
    summed, _ = lax.scan(one_expert, start, (expert_gate, expert_up, expert_down, combine.T))
    layer_out = (stream.astype(jnp.float32) + summed).astype(jnp.bfloat16)
    return (layer_out, new_states)
```

```python
import functools
import jax
import jax.numpy as jnp
from jax import lax
from jax.experimental import pallas as pl
from jax.experimental.pallas import tpu as pltpu
from jax.sharding import PartitionSpec as P

HEADS = 4
GROUPS = 4
TOP = 2
EPS = 1e-6
TAU = 16.0
MESH = pl.DeviceIdType.MESH
BF16 = jnp.bfloat16
F32 = jnp.float32
NT = (((1,), (1,)), ((), ()))
NN = (((1,), (0,)), ((), ()))
TN = (((0,), (0,)), ((), ()))


def mm(a, b, dims=NN, precision=None):
    return lax.dot_general(a, b, dims, precision=precision, preferred_element_type=F32)


def kernel(
    N,
    res_h, st_h, g1_h, wq_h, wk_h, wv_h, wg_h, wl_h, wd_h, bias_h, hg_h, wo_h, g2_h,
    rt_h, gl_h, el_h, eg_h, eu_h, ed_h,
    out_ref, ns_h,
    res, st, g1, wqk, wvg, wd, bias, hg, wo, g2, rt, gl, el, eg, eu, ed,
    g1f, g2f, xb, pj, rq, decb, cols, mx, mb, ff, ch, sb, eb, db, rb, strm,
    lsem, ssem, rsem, r1, r3, r4, osem,
):
    me = lax.axis_index("ep")
    C = N // 2
    z, c = me // 2, lax.rem(me, 2)
    T = res.shape[0]
    far = [C // 2] + [s * d for d in range(C // 2 - 1, 0, -1) for s in (1, -1)]
    near = far[::-1]

    def chip(o):
        return lax.rem(z + (o + C), C)

    barrier = pltpu.get_barrier_semaphore()
    for d in range(1, N):
        pl.semaphore_signal(barrier, inc=1, device_id={"ep": lax.rem(me + d, N)}, device_id_type=MESH)

    half = pl.multiple_of(c * 1024, 1024)
    hrow = pl.multiple_of(c * 8, 8)
    loads = [
        (res_h, res), (g1_h, g1), (g2_h, g2), (hg_h, hg), (rt_h, rt), (gl_h, gl), (el_h, el),
        (bias_h.at[pl.ds(hrow, 8)], bias), (wd_h.at[:, pl.ds(half, 1024)], wd),
        (wq_h, wqk.at[pl.ds(0, 64)]), (wk_h, wqk.at[pl.ds(64, 64)]), (wl_h, wqk.at[pl.ds(128, 16)]),
        (wv_h, wvg.at[:, pl.ds(0, 128)]), (wg_h, wvg.at[:, pl.ds(128, 128)]),
        (st_h, st), (wo_h, wo), (eg_h.at[0], eg), (eu_h.at[0], eu), (ed_h.at[0], ed),
    ]
    cps = [pltpu.make_async_copy(s, d, lsem.at[i]) for i, (s, d) in enumerate(loads)]
    for cp in cps:
        cp.start()
    for cp in cps[:9]:
        cp.wait()

    xb[me] = res[...]
    g1f[...] = g1[...].astype(F32)
    g2f[...] = g2[...].astype(F32)

    routes = rt[...]
    gexp = jnp.exp(gl[...])
    gprob = gexp / jnp.sum(gexp, axis=0, keepdims=True)
    per_group = N // GROUPS
    grow = lax.broadcasted_iota(jnp.int32, gprob.shape, 0)
    lo = grow * per_group
    first = jnp.broadcast_to(routes[0:1], gprob.shape)
    inside = (first >= lo) & (first < lo + per_group)
    gpick = jnp.sum(jnp.where(inside, gprob, 0.0), axis=0, keepdims=True)
    eexp = jnp.exp(el[...])
    weight = eexp / jnp.sum(eexp, axis=0, keepdims=True) * gpick
    before = (
        lax.broadcasted_iota(jnp.int32, (T, T), 0) < lax.broadcasted_iota(jnp.int32, (T, T), 1)
    ).astype(BF16)
    slots_all = 2 * N
    row = lax.broadcasted_iota(jnp.int32, (slots_all, T), 0)
    expert = lax.shift_right_logical(row, 1)
    r0 = jnp.broadcast_to(routes[0:1], (slots_all, T))
    r1_ = jnp.broadcast_to(routes[1:2], (slots_all, T))
    hit = jnp.where((r0 == expert) | (r1_ == expert), 1.0, 0.0)
    slot = mm(hit.astype(BF16), before)
    parity = (row - 2 * expert).astype(F32)
    ch[...] = jnp.where(slot == parity, hit, 0.0)
    my_hit = jnp.where(routes == me, 1.0, 0.0)
    share = jnp.sum(weight * my_hit, axis=0, keepdims=True)
    mine = jnp.sum(my_hit, axis=0, keepdims=True)
    my_slot = mm(jnp.broadcast_to(mine, (8, T)).astype(BF16), before)
    srow = lax.broadcasted_iota(jnp.int32, (8, T), 0).astype(F32)
    rw = jnp.sum(jnp.where(my_slot == srow, jnp.broadcast_to(mine * share, (8, T)), 0.0), axis=1, keepdims=True)

    pl.semaphore_wait(barrier, N - 1)

    def remote(src, dst, send, recv, j):
        return pltpu.make_async_remote_copy(
            src_ref=src, dst_ref=dst, send_sem=send, recv_sem=recv, device_id={"ep": j}, device_id_type=MESH
        )

    def spread(src, buf, stage, sem):
        for o in far:
            for cc in (0, 1):
                remote(src, buf.at[me], ssem.at[stage], sem.at[z], 2 * chip(o) + cc).start()
        remote(src, buf.at[me], ssem.at[stage], sem.at[z], 2 * z + 1 - c).start()

    def arrived(buf, sem, o):
        zz = chip(o)
        ref = buf.at[pl.ds(2 * zz, 2)] if o else buf.at[2 * zz]
        remote(ref, ref, sem.at[zz], sem.at[zz], me).wait_recv()
        return zz

    spread(res, xb, 0, r1)
    for cp in cps[9:14]:
        cp.wait()
    ssq = jnp.zeros((T, 256), F32)
    vg = jnp.zeros((T, 256), F32)
    qk = jnp.zeros((T, 144), F32)
    for o in [0] + near:
        zz = arrived(xb, r1, o)
        x = jnp.concatenate([xb[2 * zz], xb[2 * zz + 1]], axis=1).astype(F32)
        gain = jnp.concatenate([g1f[pl.ds(2 * zz, 1)], g1f[pl.ds(2 * zz + 1, 1)]], axis=1)
        ssq = ssq + x * x
        y = (x * gain).astype(BF16)
        at = pl.multiple_of(zz * 256, 256)
        vg = vg + mm(y, wvg[pl.ds(at, 256), :])
        qk = qk + mm(y, wqk[:, pl.ds(at, 256)], NT)
    scale = lax.rsqrt(jnp.sum(ssq, axis=1, keepdims=True) * (1.0 / (128 * N)) + EPS)
    vg = (vg * scale).astype(BF16).astype(F32)
    low = qk[:, 128:144] * scale
    qk = (qk[:, :128] * scale).astype(BF16).astype(F32)

    for s in range(T):
        pj[s, 0:1] = vg[s : s + 1, :128]
        pj[s, 1:2] = vg[s : s + 1, 128:]
        pj[s, 2:3] = qk[s : s + 1]
    S = N // 2
    core = me // S
    mine_at = lax.rem(me, S)
    for o in far:
        s = chip(o)
        remote(pj.at[s], rq.at[mine_at], ssem.at[1], rsem.at[0], 2 * s + core).start()

    @pl.when(core != c)
    def _():
        remote(pj.at[z], rq.at[mine_at], ssem.at[1], rsem.at[0], 2 * z + core).start()

    @pl.when(core == c)
    def _():
        rq[mine_at] = pj[z]

    pick = jnp.where(lax.broadcasted_iota(jnp.int32, (T, 128), 0) == z, 1.0, 0.0)
    lowcol = mm(low, pick, TN, lax.Precision.HIGHEST)
    pre = mm(wd[...].astype(F32), lowcol, TN, lax.Precision.HIGHEST)
    bcol = bias[...].T
    for b in range(8):
        v = pre[b * 128 : (b + 1) * 128] + bcol[:, b : b + 1]
        ls = jnp.minimum(v, 0.0) - jnp.log(1.0 + jnp.exp(-jnp.abs(v)))
        decb[b * 128 : (b + 1) * 128] = jnp.exp(ls * (1.0 / TAU))
    cps[14].wait()

    @pl.when(core == c)
    def _():
        ref = rq.at[pl.ds(0, S - 1)]
        remote(ref, ref, rsem.at[0], rsem.at[0], me).wait_recv()

    @pl.when(core != c)
    def _():
        remote(rq, rq, rsem.at[0], rsem.at[0], me).wait_recv()

    allv = rq[...]
    val = allv[:, 0, :]
    gat = allv[:, 1, :]
    ct = allv[:, 2, :].T
    cols[:, 0:16] = ct
    prod = ct[0:64] * ct[64:128]
    dotqk = jnp.sum(prod, axis=0, keepdims=True)
    lane = lax.broadcasted_iota(jnp.int32, (1, 16), 1)
    sub8 = lax.broadcasted_iota(jnp.int32, (8, 128), 0)
    mixed = []
    for j in range(2):
        acc = [jnp.zeros((8, 128), F32) for _ in range(8)]
        for i in range(8):
            qd = jnp.broadcast_to(ct[0:64, 8 * j + i : 8 * j + i + 1], (64, 128)) * decb[j * 512 + i * 64 : j * 512 + (i + 1) * 64]
            for k in range(8):
                q8 = qd[8 * k : 8 * k + 8]
                r = i * 64 + 8 * k
                for l in range(8):
                    acc[l] = acc[l] + q8 * st[j, r : r + 8, 128 * l : 128 * l + 128]
        read = jnp.zeros((8, 128), F32)
        for l in range(8):
            read = jnp.where(sub8 == l, jnp.sum(acc[l], axis=0, keepdims=True), read)
        sqk = jnp.sum(jnp.where((lane >= 8 * j) & (lane < 8 * j + 8), dotqk, 0.0), axis=1, keepdims=True)
        read = (read + sqk * val[8 * j : 8 * j + 8]) * (512 ** -0.5)
        tot = jnp.sum(jnp.sum(read * read, axis=1, keepdims=True), axis=0, keepdims=True)
        nrm = lax.rsqrt(tot * (1.0 / 1024) + EPS)
        g = gat[8 * j : 8 * j + 8]
        mixed.append(read * nrm * hg[...].astype(F32) * (g / (1.0 + jnp.exp(-g))))
    mixed = jnp.concatenate(mixed, axis=0).astype(BF16)
    mx[...] = mixed
    mb[me] = mixed
    spread(mx, mb, 2, r3)

    for j in range(2):
        for i in range(8):
            kc = jnp.broadcast_to(ct[64:128, 8 * j + i : 8 * j + i + 1], (64, 128))
            for k in range(8):
                r = i * 64 + 8 * k
                d8 = decb[j * 512 + r : j * 512 + r + 8]
                k8 = kc[8 * k : 8 * k + 8]
                for l in range(8):
                    sl = (j, slice(r, r + 8), slice(128 * l, 128 * l + 128))
                    st[sl] = st[sl] * d8 + k8 * val[8 * j + l : 8 * j + l + 1]
    outcp = pltpu.make_async_copy(st, ns_h, osem.at[0])
    outcp.start()
    cps[15].wait()
    for o in [0] + near:
        arrived(mb, r3, o)
    PITCH = 17
    for s in range(T):
        for cc in range(2):
            base = cc * PITCH * T + s * PITCH
            ff[base : base + 16] = mb[2 * s + cc].astype(F32)
    lhs = []
    for kb in range(N):
        base = (kb // 16) * PITCH * T + kb % 16
        lhs.append(ff[pl.ds(base, T, stride=PITCH), :].astype(BF16))
    branch = mm(jnp.concatenate(lhs, axis=1), wo[...]).astype(BF16).astype(F32)
    stream = (res[...].astype(F32) + branch).astype(BF16)
    strm[...] = stream

    picked = mm(ch[...].astype(BF16), stream)
    sb[...] = picked.reshape(N, 2, 128).astype(sb.dtype)
    for o in far:
        for cc in (0, 1):
            j = 2 * chip(o) + cc
            remote(sb.at[j], eb.at[me], ssem.at[3], r4.at[z], j).start()
    remote(sb.at[2 * z + 1 - c], eb.at[me], ssem.at[3], r4.at[z], 2 * z + 1 - c).start()
    eb[me] = sb[me]
    for cp in cps[16:18]:
        cp.wait()
    ssq = jnp.zeros((2, 256), F32)
    ga = jnp.zeros((2, 512), F32)
    up = jnp.zeros((2, 512), F32)
    for o in [0] + near:
        zz = arrived(eb, r4, o)
        x = jnp.concatenate([eb[2 * zz], eb[2 * zz + 1]], axis=1).astype(F32)
        gain = jnp.concatenate([g2f[pl.ds(2 * zz, 1)], g2f[pl.ds(2 * zz + 1, 1)]], axis=1)
        ssq = ssq + x * x
        y = (x * gain).astype(BF16)
        at = pl.multiple_of(zz * 256, 256)
        ga = ga + mm(y, eg[pl.ds(at, 256), :])
        up = up + mm(y, eu[pl.ds(at, 256), :])
    scale = lax.rsqrt(jnp.sum(ssq, axis=1, keepdims=True) * (1.0 / (128 * N)) + EPS)
    ga = ga * scale
    act = (ga / (1.0 + jnp.exp(-ga)) * (up * scale) * rw[0:2]).astype(BF16)

    cps[18].wait()
    for o in far + [0]:
        zz = chip(o)
        at = pl.multiple_of(zz * 256, 256)
        rows = mm(act, ed[:, pl.ds(at, 256)])
        for cc in (0, 1):
            db[2 * zz + cc] = rows[:, 128 * cc : 128 * cc + 128].astype(BF16).astype(db.dtype)
            if o:
                remote(db.at[2 * zz + cc], rb.at[me], ssem.at[4], rsem.at[1], 2 * zz + cc).start()
    remote(db.at[2 * z + 1 - c], rb.at[me], ssem.at[4], rsem.at[1], 2 * z + 1 - c).start()
    rb[me] = db[me]
    ref = rb.at[pl.ds(0, N - 1)]
    remote(ref, ref, rsem.at[1], rsem.at[1], me).wait_recv()
    back = mm(ch[...].astype(BF16), rb[...].reshape(2 * N, 128).astype(BF16), TN)
    out_ref[...] = (strm[...].astype(F32) + back).astype(BF16)

    for stage, ref in ((0, xb.at[pl.ds(0, N - 1)]), (2, mb.at[pl.ds(0, N - 1)]), (3, eb.at[pl.ds(0, N - 1)]), (4, rb.at[pl.ds(0, N - 1)])):
        remote(ref, ref, ssem.at[stage], ssem.at[stage], me).wait_send()

    @pl.when(core == c)
    def _():
        ref = rq.at[pl.ds(0, S - 1)]
        remote(ref, ref, ssem.at[1], ssem.at[1], me).wait_send()

    @pl.when(core != c)
    def _():
        remote(rq, rq, ssem.at[1], ssem.at[1], me).wait_send()

    outcp.wait()


def per_device(N, residual, head_states, first_gain, w_query, w_key, w_value, w_gate, w_low, w_decay, decay_bias,
               head_gain, w_output, second_gain, routes, group_logits, expert_logits, expert_gate, expert_up, expert_down):
    args = (
        residual, head_states, first_gain.reshape(-1, 128), w_query.T, w_key.T, w_value, w_gate, w_low.T, w_decay,
        decay_bias.reshape(-1, 128), head_gain.reshape(-1, 128), w_output, second_gain.reshape(-1, 128),
        routes.T, group_logits.T, expert_logits.T, expert_gate, expert_up, expert_down,
    )
    V = pltpu.VMEM
    D = 128 * N
    SB = BF16
    scratch = [
        V((16, 128), BF16), V((2, 512, 1024), F32), V((N, 128), BF16), V((144, D), BF16), V((D, 256), BF16),
        V((16, 1024), BF16), V((8, 128), F32), V((8, 128), BF16), V((D, 128), BF16), V((N, 128), BF16),
        V((2, 16), jnp.int32), V((4, 16), F32), V((2, 16), F32), V((D, 512), BF16), V((D, 512), BF16), V((512, D), BF16),
        V((N, 128), F32), V((N, 128), F32), V((N, 16, 128), BF16), V((16, 4, 128), F32), V((16, 4, 128), F32),
        V((1024, 128), F32), V((128, 128), F32), V((16, 128), BF16), V((N, 16, 128), BF16), V((2 * 17 * 16, 128), F32),
        V((2 * N, 16), F32), V((N, 2, 128), SB), V((N, 2, 128), SB), V((N, 2, 128), SB), V((N, 2, 128), SB), V((16, 128), BF16),
        pltpu.SemaphoreType.DMA((19,)), pltpu.SemaphoreType.DMA((5,)), pltpu.SemaphoreType.DMA((2,)),
        pltpu.SemaphoreType.DMA((N // 2,)), pltpu.SemaphoreType.DMA((N // 2,)), pltpu.SemaphoreType.DMA((N // 2,)),
        pltpu.SemaphoreType.DMA((1,)),
    ]
    return pl.pallas_call(
        functools.partial(kernel, N),
        out_shape=(jax.ShapeDtypeStruct(residual.shape, BF16), jax.ShapeDtypeStruct(head_states.shape, F32)),
        in_specs=[pl.BlockSpec(memory_space=pl.ANY)] * len(args),
        out_specs=(pl.BlockSpec(memory_space=pltpu.VMEM), pl.BlockSpec(memory_space=pl.ANY)),
        scratch_shapes=scratch,
        compiler_params=pltpu.CompilerParams(collective_id=0, has_side_effects=True, vmem_limit_bytes=56 * 1024 * 1024),
    )(*args)


def solution(mesh):
    N = mesh.shape["ep"]
    return jax.shard_map(
        functools.partial(per_device, N),
        mesh=mesh,
        in_specs=(
            P("grp", "ep"), P(("grp", "ep"), None, None), P(), P(None, "ep"), P(None, "ep"), P(None, "ep"), P(None, "ep"),
            P(), P(), P(), P(), P(None, "ep"), P(), P("grp", None), P("grp", None), P("grp", None),
            P("ep", None, None), P("ep", None, None), P("ep", None, None),
        ),
        out_specs=(P("grp", "ep"), P(("grp", "ep"), None, None)),
        check_vma=False,
    )
```

```python
import functools
import jax
import jax.numpy as jnp
from jax import lax
from jax.experimental import pallas as pl
from jax.experimental.pallas import tpu as pltpu
from jax.sharding import PartitionSpec as P

HEADS = 4
GROUPS = 4
TOP = 2
EPS = 1e-6
TAU = 16.0
MESH = pl.DeviceIdType.MESH
BF16 = jnp.bfloat16
F32 = jnp.float32
NT = (((1,), (1,)), ((), ()))
NN = (((1,), (0,)), ((), ()))
TN = (((0,), (0,)), ((), ()))


def mm(a, b, dims=NN, precision=None):
    return lax.dot_general(a, b, dims, precision=precision, preferred_element_type=F32)


def kernel(
    N,
    res_h, st_h, g1_h, wq_h, wk_h, wv_h, wg_h, wl_h, wd_h, bias_h, hg_h, wo_h, g2_h,
    rt_h, gl_h, el_h, eg_h, eu_h, ed_h,
    out_ref, st,
    res, g1, wqk, wvg, wd, bias, hg, wo, g2, rt, gl, el, eg, eu, ed,
    g1f, g2f, xb, pj, rq, decb, cols, mx, mb, ff, ch, sb, eb, db, rb, strm,
    lsem, ssem, rsem, r1, r3, r4, osem,
):
    me = lax.axis_index("ep")
    C = N // 2
    z, c = me // 2, lax.rem(me, 2)
    T = res.shape[0]
    far = [C // 2] + [s * d for d in range(C // 2 - 1, 0, -1) for s in (1, -1)]
    near = far[::-1]

    def chip(o):
        return lax.rem(z + (o + C), C)

    barrier = pltpu.get_barrier_semaphore()
    reach = C // 4
    close = [o for o in near if abs(o) <= reach]
    for o in close:
        for cc in (0, 1):
            pl.semaphore_signal(barrier, inc=1, device_id={"ep": 2 * chip(o) + cc}, device_id_type=MESH)
    pl.semaphore_signal(barrier, inc=1, device_id={"ep": 2 * z + 1 - c}, device_id_type=MESH)

    half = pl.multiple_of(c * 1024, 1024)
    hrow = pl.multiple_of(c * 8, 8)
    loads = [
        (res_h, res), (g1_h, g1), (g2_h, g2), (hg_h, hg), (rt_h, rt), (gl_h, gl), (el_h, el),
        (bias_h.at[pl.ds(hrow, 8)], bias), (wd_h.at[:, pl.ds(half, 1024)], wd),
        (wq_h, wqk.at[pl.ds(0, 64)]), (wk_h, wqk.at[pl.ds(64, 64)]), (wl_h, wqk.at[pl.ds(128, 16)]),
        (wv_h, wvg.at[:, pl.ds(0, 128)]), (wg_h, wvg.at[:, pl.ds(128, 128)]),
        (st_h, st), (wo_h, wo), (eg_h.at[0], eg), (eu_h.at[0], eu), (ed_h.at[0], ed),
    ]
    cps = [pltpu.make_async_copy(s, d, lsem.at[i]) for i, (s, d) in enumerate(loads)]
    for cp in cps[:14]:
        cp.start()
    for cp in cps[:9]:
        cp.wait()

    xb[me] = res[...]
    g1f[...] = g1[...].astype(F32)
    g2f[...] = g2[...].astype(F32)

    routes = rt[...]
    gexp = jnp.exp(gl[...])
    gprob = gexp / jnp.sum(gexp, axis=0, keepdims=True)
    per_group = N // GROUPS
    grow = lax.broadcasted_iota(jnp.int32, gprob.shape, 0)
    lo = grow * per_group
    first = jnp.broadcast_to(routes[0:1], gprob.shape)
    inside = (first >= lo) & (first < lo + per_group)
    gpick = jnp.sum(jnp.where(inside, gprob, 0.0), axis=0, keepdims=True)
    eexp = jnp.exp(el[...])
    weight = eexp / jnp.sum(eexp, axis=0, keepdims=True) * gpick
    before = (
        lax.broadcasted_iota(jnp.int32, (T, T), 0) < lax.broadcasted_iota(jnp.int32, (T, T), 1)
    ).astype(BF16)
    slots_all = 2 * N
    row = lax.broadcasted_iota(jnp.int32, (slots_all, T), 0)
    expert = lax.shift_right_logical(row, 1)
    r0 = jnp.broadcast_to(routes[0:1], (slots_all, T))
    r1_ = jnp.broadcast_to(routes[1:2], (slots_all, T))
    hit = jnp.where((r0 == expert) | (r1_ == expert), 1.0, 0.0)
    slot = mm(hit.astype(BF16), before)
    parity = (row - 2 * expert).astype(F32)
    ch[...] = jnp.where(slot == parity, hit, 0.0)
    my_hit = jnp.where(routes == me, 1.0, 0.0)
    share = jnp.sum(weight * my_hit, axis=0, keepdims=True)
    mine = jnp.sum(my_hit, axis=0, keepdims=True)
    my_slot = mm(jnp.broadcast_to(mine, (8, T)).astype(BF16), before)
    srow = lax.broadcasted_iota(jnp.int32, (8, T), 0).astype(F32)
    rw = jnp.sum(jnp.where(my_slot == srow, jnp.broadcast_to(mine * share, (8, T)), 0.0), axis=1, keepdims=True)

    pl.semaphore_wait(barrier, 2 * len(close) + 1)

    def remote(src, dst, send, recv, j):
        return pltpu.make_async_remote_copy(
            src_ref=src, dst_ref=dst, send_sem=send, recv_sem=recv, device_id={"ep": j}, device_id_type=MESH
        )


    def arrived(buf, sem, o):
        zz = chip(o)
        ref = buf.at[pl.ds(2 * zz, 2)] if o else buf.at[2 * zz]
        remote(ref, ref, sem.at[zz], sem.at[zz], me).wait_recv()
        return zz

    for o in close[::-1]:
        for cc in (0, 1):
            remote(res, xb.at[me], ssem.at[0], r1.at[z], 2 * chip(o) + cc).start()
    remote(res, xb.at[me], ssem.at[0], r1.at[z], 2 * z + 1 - c).start()
    for o in close + [0]:
        zz = arrived(xb, r1, o)
        if 0 < o <= reach or -reach < o < 0:
            to = chip(-reach if o > 0 else reach)
            for cc in (0, 1):
                blk = xb.at[2 * zz + c]
                remote(blk, blk, ssem.at[0], r1.at[zz], 2 * to + cc).start()
    for cp in cps[14:]:
        cp.start()
    for cp in cps[9:14]:
        cp.wait()
    ssq = jnp.zeros((T, 256), F32)
    vg = jnp.zeros((T, 256), F32)
    qk = jnp.zeros((T, 144), F32)
    for o in [0] + near:
        zz = chip(o) if abs(o) <= reach else arrived(xb, r1, o)
        x = jnp.concatenate([xb[2 * zz], xb[2 * zz + 1]], axis=1).astype(F32)
        gain = jnp.concatenate([g1f[pl.ds(2 * zz, 1)], g1f[pl.ds(2 * zz + 1, 1)]], axis=1)
        ssq = ssq + x * x
        y = (x * gain).astype(BF16)
        at = pl.multiple_of(zz * 256, 256)
        vg = vg + mm(y, wvg[pl.ds(at, 256), :])
        qk = qk + mm(y, wqk[:, pl.ds(at, 256)], NT)
    scale = lax.rsqrt(jnp.sum(ssq, axis=1, keepdims=True) * (1.0 / (128 * N)) + EPS)
    vg = (vg * scale).astype(BF16).astype(F32)
    low = qk[:, 128:144] * scale
    qk = (qk[:, :128] * scale).astype(BF16).astype(F32)

    for s in range(T):
        pj[s, 0:1] = vg[s : s + 1, :128]
        pj[s, 1:2] = vg[s : s + 1, 128:]
        pj[s, 2:3] = qk[s : s + 1]
    S = N // 2
    core = me // S
    mine_at = lax.rem(me, S)
    for o in far:
        s = chip(o)
        remote(pj.at[s], rq.at[mine_at], ssem.at[1], rsem.at[0], 2 * s + core).start()

    @pl.when(core != c)
    def _():
        remote(pj.at[z], rq.at[mine_at], ssem.at[1], rsem.at[0], 2 * z + core).start()

    @pl.when(core == c)
    def _():
        rq[mine_at] = pj[z]

    pick = jnp.where(lax.broadcasted_iota(jnp.int32, (T, 128), 0) == z, 1.0, 0.0)
    lowcol = mm(low, pick, TN, lax.Precision.HIGHEST)
    pre = mm(wd[...].astype(F32), lowcol, TN, lax.Precision.HIGHEST)
    bcol = bias[...].T
    for b in range(8):
        v = pre[b * 128 : (b + 1) * 128] + bcol[:, b : b + 1]
        ls = jnp.minimum(v, 0.0) - jnp.log(1.0 + jnp.exp(-jnp.abs(v)))
        decb[b * 128 : (b + 1) * 128] = jnp.exp(ls * (1.0 / TAU))
    cps[14].wait()

    @pl.when(core == c)
    def _():
        ref = rq.at[pl.ds(0, S - 1)]
        remote(ref, ref, rsem.at[0], rsem.at[0], me).wait_recv()

    @pl.when(core != c)
    def _():
        remote(rq, rq, rsem.at[0], rsem.at[0], me).wait_recv()

    allv = rq[...]
    val = allv[:, 0, :]
    gat = allv[:, 1, :]
    ct = allv[:, 2, :].T
    cols[:, 0:16] = ct
    prod = ct[0:64] * ct[64:128]
    dotqk = jnp.sum(prod, axis=0, keepdims=True)
    lane = lax.broadcasted_iota(jnp.int32, (1, 16), 1)
    sub8 = lax.broadcasted_iota(jnp.int32, (8, 128), 0)
    mixed = []
    for j in range(2):
        acc = [jnp.zeros((8, 128), F32) for _ in range(8)]
        for i in range(8):
            qd = jnp.broadcast_to(ct[0:64, 8 * j + i : 8 * j + i + 1], (64, 128)) * decb[j * 512 + i * 64 : j * 512 + (i + 1) * 64]
            for k in range(8):
                q8 = qd[8 * k : 8 * k + 8]
                r = i * 64 + 8 * k
                for l in range(8):
                    acc[l] = acc[l] + q8 * st[j, r : r + 8, 128 * l : 128 * l + 128]
        read = jnp.zeros((8, 128), F32)
        for l in range(8):
            read = jnp.where(sub8 == l, jnp.sum(acc[l], axis=0, keepdims=True), read)
        sqk = jnp.sum(jnp.where((lane >= 8 * j) & (lane < 8 * j + 8), dotqk, 0.0), axis=1, keepdims=True)
        read = (read + sqk * val[8 * j : 8 * j + 8]) * (512 ** -0.5)
        tot = jnp.sum(jnp.sum(read * read, axis=1, keepdims=True), axis=0, keepdims=True)
        nrm = lax.rsqrt(tot * (1.0 / 1024) + EPS)
        g = gat[8 * j : 8 * j + 8]
        mixed.append(read * nrm * hg[...].astype(F32) * (g / (1.0 + jnp.exp(-g))))
    mixed = jnp.concatenate(mixed, axis=0).astype(BF16)
    mx[...] = mixed
    mb[me] = mixed
    for o in far:
        remote(mx, mb.at[me], ssem.at[2], r3.at[z], 2 * chip(o) + c).start()
    remote(mx, mb.at[me], ssem.at[2], rsem.at[2], 2 * z + 1 - c).start()

    for j in range(2):
        for i in range(8):
            kc = jnp.broadcast_to(ct[64:128, 8 * j + i : 8 * j + i + 1], (64, 128))
            for k in range(8):
                r = i * 64 + 8 * k
                d8 = decb[j * 512 + r : j * 512 + r + 8]
                k8 = kc[8 * k : 8 * k + 8]
                for l in range(8):
                    sl = (j, slice(r, r + 8), slice(128 * l, 128 * l + 128))
                    st[sl] = st[sl] * d8 + k8 * val[8 * j + l : 8 * j + l + 1]
    cps[15].wait()
    for o in near:
        zz = chip(o)
        blk = mb.at[2 * zz + c]
        remote(blk, blk, r3.at[zz], r3.at[zz], me).wait_recv()
        remote(blk, blk, ssem.at[2], rsem.at[2], 2 * z + 1 - c).start()
    PITCH = 17
    for s in range(T):
        ff[c, s * PITCH : s * PITCH + 16] = mb[2 * s + c].astype(F32)
    half_mb = mb.at[pl.ds(0, C)]
    remote(half_mb, half_mb, rsem.at[2], rsem.at[2], me).wait_recv()
    for s in range(T):
        ff[1 - c, s * PITCH : s * PITCH + 16] = mb[2 * s + 1 - c].astype(F32)
    lhs = []
    for kb in range(N):
        lhs.append(ff[kb // 16, pl.ds(kb % 16, T, stride=PITCH), :].astype(BF16))
    branch = mm(jnp.concatenate(lhs, axis=1), wo[...]).astype(BF16).astype(F32)
    stream = (res[...].astype(F32) + branch).astype(BF16)
    strm[...] = stream

    picked = mm(ch[...].astype(BF16), stream)
    sb[...] = picked.reshape(N, 2, 128).astype(sb.dtype)
    for o in far:
        for cc in (0, 1):
            j = 2 * chip(o) + cc
            remote(sb.at[j], eb.at[me], ssem.at[3], r4.at[z], j).start()
    remote(sb.at[2 * z + 1 - c], eb.at[me], ssem.at[3], r4.at[z], 2 * z + 1 - c).start()
    eb[me] = sb[me]
    for cp in cps[16:18]:
        cp.wait()
    ssq = jnp.zeros((2, 256), F32)
    ga = jnp.zeros((2, 512), F32)
    up = jnp.zeros((2, 512), F32)
    for o in [0] + near:
        zz = arrived(eb, r4, o)
        x = jnp.concatenate([eb[2 * zz], eb[2 * zz + 1]], axis=1).astype(F32)
        gain = jnp.concatenate([g2f[pl.ds(2 * zz, 1)], g2f[pl.ds(2 * zz + 1, 1)]], axis=1)
        ssq = ssq + x * x
        y = (x * gain).astype(BF16)
        at = pl.multiple_of(zz * 256, 256)
        ga = ga + mm(y, eg[pl.ds(at, 256), :])
        up = up + mm(y, eu[pl.ds(at, 256), :])
    scale = lax.rsqrt(jnp.sum(ssq, axis=1, keepdims=True) * (1.0 / (128 * N)) + EPS)
    ga = ga * scale
    act = (ga / (1.0 + jnp.exp(-ga)) * (up * scale) * rw[0:2]).astype(BF16)

    cps[18].wait()
    for o in far + [0]:
        zz = chip(o)
        at = pl.multiple_of(zz * 256, 256)
        rows = mm(act, ed[:, pl.ds(at, 256)])
        for cc in (0, 1):
            db[2 * zz + cc] = rows[:, 128 * cc : 128 * cc + 128].astype(BF16).astype(db.dtype)
            if o:
                remote(db.at[2 * zz + cc], rb.at[me], ssem.at[4], rsem.at[1], 2 * zz + cc).start()
    remote(db.at[2 * z + 1 - c], rb.at[me], ssem.at[4], rsem.at[1], 2 * z + 1 - c).start()
    rb[me] = db[me]
    ref = rb.at[pl.ds(0, N - 1)]
    remote(ref, ref, rsem.at[1], rsem.at[1], me).wait_recv()
    back = mm(ch[...].astype(BF16), rb[...].reshape(2 * N, 128).astype(BF16), TN)
    out_ref[...] = (strm[...].astype(F32) + back).astype(BF16)

    for stage, ref in ((0, xb.at[pl.ds(0, N - 1)]), (2, mb.at[pl.ds(0, N - 1)]), (3, eb.at[pl.ds(0, N - 1)]), (4, rb.at[pl.ds(0, N - 1)])):
        remote(ref, ref, ssem.at[stage], ssem.at[stage], me).wait_send()

    @pl.when(core == c)
    def _():
        ref = rq.at[pl.ds(0, S - 1)]
        remote(ref, ref, ssem.at[1], ssem.at[1], me).wait_send()

    @pl.when(core != c)
    def _():
        remote(rq, rq, ssem.at[1], ssem.at[1], me).wait_send()


def per_device(N, residual, head_states, first_gain, w_query, w_key, w_value, w_gate, w_low, w_decay, decay_bias,
               head_gain, w_output, second_gain, routes, group_logits, expert_logits, expert_gate, expert_up, expert_down):
    args = (
        residual, head_states, first_gain.reshape(-1, 128), w_query.T, w_key.T, w_value, w_gate, w_low.T, w_decay,
        decay_bias.reshape(-1, 128), head_gain.reshape(-1, 128), w_output, second_gain.reshape(-1, 128),
        routes.T, group_logits.T, expert_logits.T, expert_gate, expert_up, expert_down,
    )
    V = pltpu.VMEM
    args = tuple(pltpu.with_memory_space_constraint(a, pltpu.HBM) for a in args)
    D = 128 * N
    SB = BF16
    scratch = [
        V((16, 128), BF16), V((N, 128), BF16), V((144, D), BF16), V((D, 256), BF16),
        V((16, 1024), BF16), V((8, 128), F32), V((8, 128), BF16), V((D, 128), BF16), V((N, 128), BF16),
        V((2, 16), jnp.int32), V((4, 16), F32), V((2, 16), F32), V((D, 512), BF16), V((D, 512), BF16), V((512, D), BF16),
        V((N, 128), F32), V((N, 128), F32), V((N, 16, 128), BF16), V((16, 4, 128), F32), V((16, 4, 128), F32),
        V((1024, 128), F32), V((128, 128), F32), V((16, 128), BF16), V((N, 16, 128), BF16), V((2, 17 * 16, 128), F32),
        V((2 * N, 16), F32), V((N, 2, 128), SB), V((N, 2, 128), SB), V((N, 2, 128), SB), V((N, 2, 128), SB), V((16, 128), BF16),
        pltpu.SemaphoreType.DMA((19,)), pltpu.SemaphoreType.DMA((5,)), pltpu.SemaphoreType.DMA((3,)),
        pltpu.SemaphoreType.DMA((N // 2,)), pltpu.SemaphoreType.DMA((N // 2,)), pltpu.SemaphoreType.DMA((N // 2,)),
        pltpu.SemaphoreType.DMA((1,)),
    ]
    lo, ns = pl.pallas_call(
        functools.partial(kernel, N),
        out_shape=(jax.ShapeDtypeStruct(residual.shape, BF16), jax.ShapeDtypeStruct(head_states.shape, F32)),
        in_specs=[pl.BlockSpec(memory_space=pl.ANY)] * len(args),
        out_specs=(pl.BlockSpec(memory_space=pltpu.VMEM), pl.BlockSpec(memory_space=pltpu.VMEM)),
        scratch_shapes=scratch,
        compiler_params=pltpu.CompilerParams(collective_id=0, has_side_effects=True, vmem_limit_bytes=40 * 1024 * 1024),
    )(*args)

    def tail(lo_ref, ns_ref, o_ref, on_ref, sem):
        cps = [pltpu.make_async_copy(lo_ref, o_ref, sem.at[8])]
        for i in range(8):
            at = (i // 4, pl.ds(128 * (i % 4), 128))
            cps.append(pltpu.make_async_copy(ns_ref.at[at], on_ref.at[at], sem.at[i]))
        for cp in cps:
            cp.start()
        for cp in cps:
            cp.wait()

    return pl.pallas_call(
        tail,
        out_shape=(jax.ShapeDtypeStruct(residual.shape, BF16), jax.ShapeDtypeStruct(head_states.shape, F32)),
        in_specs=[pl.BlockSpec(memory_space=pltpu.VMEM), pl.BlockSpec(memory_space=pltpu.VMEM)],
        out_specs=(pl.BlockSpec(memory_space=pl.ANY), pl.BlockSpec(memory_space=pl.ANY)),
        scratch_shapes=[pltpu.SemaphoreType.DMA((9,))],
        compiler_params=pltpu.CompilerParams(vmem_limit_bytes=16 * 1024 * 1024),
    )(lo, ns)


def solution(mesh):
    N = mesh.shape["ep"]
    return jax.shard_map(
        functools.partial(per_device, N),
        mesh=mesh,
        in_specs=(
            P("grp", "ep"), P(("grp", "ep"), None, None), P(), P(None, "ep"), P(None, "ep"), P(None, "ep"), P(None, "ep"),
            P(), P(), P(), P(), P(None, "ep"), P(), P("grp", None), P("grp", None), P("grp", None),
            P("ep", None, None), P("ep", None, None), P("ep", None, None),
        ),
        out_specs=(P("grp", "ep"), P(("grp", "ep"), None, None)),
        check_vma=False,
    )
```

```python
import functools
import jax
import jax.numpy as jnp
from jax import lax
from jax.experimental import pallas as pl
from jax.experimental.pallas import tpu as pltpu
from jax.sharding import PartitionSpec as P

HEADS = 4
GROUPS = 4
TOP = 2
EPS = 1e-6
TAU = 16.0
MESH = pl.DeviceIdType.MESH
BF16 = jnp.bfloat16
F32 = jnp.float32
NT = (((1,), (1,)), ((), ()))
NN = (((1,), (0,)), ((), ()))
TN = (((0,), (0,)), ((), ()))


def mm(a, b, dims=NN, precision=None):
    return lax.dot_general(a, b, dims, precision=precision, preferred_element_type=F32)


def kernel(
    N,
    res_h, st_h, g1_h, wq_h, wk_h, wv_h, wg_h, wl_h, wd_h, bias_h, hg_h, wo_h, g2_h,
    rt_h, gl_h, el_h, eg_h, eu_h, ed_h,
    out_ref, st,
    res, g1, wqk, wvg, wd, bias, hg, wo, g2, rt, gl, el, eg, eu, ed,
    g1f, g2f, xb, pj, rq, decb, cols, mx, mb, ff, ch, cht, sb, eb, db, rb, rs, ps, pr,
    lsem, ssem, rsem, r1, r3, r4, osem,
):
    me = lax.axis_index("ep")
    C = N // 2
    z, c = me // 2, lax.rem(me, 2)
    T = res.shape[0]
    far = [C // 2] + [s * d for d in range(C // 2 - 1, 0, -1) for s in (1, -1)]
    near = far[::-1]

    def chip(o):
        return lax.rem(z + (o + C), C)

    barrier = pltpu.get_barrier_semaphore()
    reach = C // 4
    close = [o for o in near if abs(o) <= reach]
    for o in close[::-1]:
        for cc in (0, 1):
            pl.semaphore_signal(barrier, inc=1, device_id={"ep": 2 * chip(o) + cc}, device_id_type=MESH)
    pl.semaphore_signal(barrier, inc=1, device_id={"ep": 2 * z + 1 - c}, device_id_type=MESH)

    half = pl.multiple_of(c * 1024, 1024)
    hrow = pl.multiple_of(c * 8, 8)
    kmine, kother = pl.multiple_of(c * 2048, 2048), pl.multiple_of(2048 - c * 2048, 2048)
    lmine, lother = pl.multiple_of(c * 128, 128), pl.multiple_of(128 - c * 128, 128)
    loads = [
        (res_h, res), (g1_h, g1), (g2_h, g2), (hg_h, hg), (rt_h, rt), (gl_h, gl), (el_h, el),
        (bias_h.at[pl.ds(hrow, 8)], bias), (wd_h.at[:, pl.ds(half, 1024)], wd),
        (wq_h, wqk.at[pl.ds(0, 64)]), (wk_h, wqk.at[pl.ds(64, 64)]), (wl_h, wqk.at[pl.ds(128, 16)]),
        (wv_h, wvg.at[:, pl.ds(0, 128)]), (wg_h, wvg.at[:, pl.ds(128, 128)]),
        (st_h, st), (wo_h.at[pl.ds(kmine, 2048)], wo.at[:, pl.ds(lmine, 128)]), (eg_h.at[0], eg), (eu_h.at[0], eu), (ed_h.at[0], ed),
    ]
    cps = [pltpu.make_async_copy(s, d, lsem.at[i]) for i, (s, d) in enumerate(loads)]
    for cp in cps[:14]:
        cp.start()
    cps[0].wait()

    xb[me] = res[...]
    pl.semaphore_wait(barrier, 2 * len(close) + 1)

    def remote(src, dst, send, recv, j):
        return pltpu.make_async_remote_copy(
            src_ref=src, dst_ref=dst, send_sem=send, recv_sem=recv, device_id={"ep": j}, device_id_type=MESH
        )


    def arrived(buf, sem, o):
        zz = chip(o)
        ref = buf.at[pl.ds(2 * zz, 2)] if o else buf.at[2 * zz]
        remote(ref, ref, sem.at[zz], sem.at[zz], me).wait_recv()
        return zz

    for o in close[::-1]:
        for cc in (0, 1):
            remote(res, xb.at[me], ssem.at[0], r1.at[z], 2 * chip(o) + cc).start()
    remote(res, xb.at[me], ssem.at[0], r1.at[z], 2 * z + 1 - c).start()
    for cp in cps[1:9]:
        cp.wait()
    g1f[...] = g1[...].astype(F32)
    g2f[...] = g2[...].astype(F32)

    routes = rt[...]
    gexp = jnp.exp(gl[...])
    gprob = gexp / jnp.sum(gexp, axis=0, keepdims=True)
    per_group = N // GROUPS
    grow = lax.broadcasted_iota(jnp.int32, gprob.shape, 0)
    lo = grow * per_group
    first = jnp.broadcast_to(routes[0:1], gprob.shape)
    inside = (first >= lo) & (first < lo + per_group)
    gpick = jnp.sum(jnp.where(inside, gprob, 0.0), axis=0, keepdims=True)
    eexp = jnp.exp(el[...])
    weight = eexp / jnp.sum(eexp, axis=0, keepdims=True) * gpick
    before = (
        lax.broadcasted_iota(jnp.int32, (T, T), 0) < lax.broadcasted_iota(jnp.int32, (T, T), 1)
    ).astype(BF16)
    slots_all = 2 * N
    row = lax.broadcasted_iota(jnp.int32, (slots_all, T), 0)
    expert = lax.shift_right_logical(row, 1)
    r0 = jnp.broadcast_to(routes[0:1], (slots_all, T))
    r1_ = jnp.broadcast_to(routes[1:2], (slots_all, T))
    hit = jnp.where((r0 == expert) | (r1_ == expert), 1.0, 0.0)
    slot = mm(hit.astype(BF16), before)
    parity = (row - 2 * expert).astype(F32)
    chv = jnp.where(slot == parity, hit, 0.0)
    ch[...] = chv.astype(BF16)
    cht[...] = chv.T.astype(BF16)
    my_hit = jnp.where(routes == me, 1.0, 0.0)
    share = jnp.sum(weight * my_hit, axis=0, keepdims=True)
    mine = jnp.sum(my_hit, axis=0, keepdims=True)
    my_slot = mm(jnp.broadcast_to(mine, (8, T)).astype(BF16), before)
    srow = lax.broadcasted_iota(jnp.int32, (8, T), 0).astype(F32)
    rw = jnp.sum(jnp.where(my_slot == srow, jnp.broadcast_to(mine * share, (8, T)), 0.0), axis=1, keepdims=True)
    my_rows = jnp.where(my_slot == srow, jnp.broadcast_to(mine, (8, T)), 0.0).astype(BF16)

    for o in close + [0]:
        zz = arrived(xb, r1, o)
        if 0 < o <= reach or -reach < o < 0:
            to = chip(-reach if o > 0 else reach)
            for cc in (0, 1):
                blk = xb.at[2 * zz + c]
                remote(blk, blk, ssem.at[0], r1.at[zz], 2 * to + cc).start()
    for cp in cps[14:]:
        cp.start()
    for cp in cps[9:14]:
        cp.wait()
    ssq = jnp.zeros((T, 256), F32)
    vg = jnp.zeros((T, 256), F32)
    qk = jnp.zeros((T, 144), F32)
    for o in [0] + near:
        zz = chip(o) if abs(o) <= reach else arrived(xb, r1, o)
        x = jnp.concatenate([xb[2 * zz], xb[2 * zz + 1]], axis=1).astype(F32)
        gain = jnp.concatenate([g1f[pl.ds(2 * zz, 1)], g1f[pl.ds(2 * zz + 1, 1)]], axis=1)
        ssq = ssq + x * x
        y = (x * gain).astype(BF16)
        at = pl.multiple_of(zz * 256, 256)
        vg = vg + mm(y, wvg[pl.ds(at, 256), :])
        qk = qk + mm(y, wqk[:, pl.ds(at, 256)], NT)
    scale = lax.rsqrt(jnp.sum(ssq, axis=1, keepdims=True) * (1.0 / (128 * N)) + EPS)
    vg = (vg * scale).astype(BF16).astype(F32)
    low = qk[:, 128:144] * scale
    qk = (qk[:, :128] * scale).astype(BF16).astype(F32)

    for s in range(T):
        pj[s, 0:1] = vg[s : s + 1, :128]
        pj[s, 1:2] = vg[s : s + 1, 128:]
        pj[s, 2:3] = qk[s : s + 1]
    S = N // 2
    core = me // S
    mine_at = lax.rem(me, S)
    for o in far:
        s = chip(o)
        remote(pj.at[s], rq.at[mine_at], ssem.at[1], rsem.at[0], 2 * s + core).start()

    @pl.when(core != c)
    def _():
        remote(pj.at[z], rq.at[mine_at], ssem.at[1], rsem.at[0], 2 * z + core).start()

    @pl.when(core == c)
    def _():
        rq[mine_at] = pj[z]

    other = 2 * z + 1 - c
    wsend = remote(wo_h.at[pl.ds(kother, 2048)], wo.at[:, pl.ds(lmine, 128)], ssem.at[5], rsem.at[3], other)
    wsend.start()
    for s in range(C):
        both = jnp.concatenate([xb[2 * s], xb[2 * s + 1]], axis=1)
        rs[s] = mm(my_rows, both)

    pick = jnp.where(lax.broadcasted_iota(jnp.int32, (T, 128), 0) == z, 1.0, 0.0)
    lowcol = mm(low, pick, TN, lax.Precision.HIGHEST)
    pre = mm(wd[...].astype(F32), lowcol, TN, lax.Precision.HIGHEST)
    bcol = bias[...].T
    for b in range(8):
        v = pre[b * 128 : (b + 1) * 128] + bcol[:, b : b + 1]
        ls = jnp.minimum(v, 0.0) - jnp.log(1.0 + jnp.exp(-jnp.abs(v)))
        decb[b * 128 : (b + 1) * 128] = jnp.exp(ls * (1.0 / TAU))
    cps[14].wait()

    @pl.when(core == c)
    def _():
        ref = rq.at[pl.ds(0, S - 1)]
        remote(ref, ref, rsem.at[0], rsem.at[0], me).wait_recv()

    @pl.when(core != c)
    def _():
        remote(rq, rq, rsem.at[0], rsem.at[0], me).wait_recv()

    allv = rq[...]
    val = allv[:, 0, :]
    gat = allv[:, 1, :]
    ct = allv[:, 2, :].T
    cols[:, 0:16] = ct
    prod = ct[0:64] * ct[64:128]
    dotqk = jnp.sum(prod, axis=0, keepdims=True)
    lane = lax.broadcasted_iota(jnp.int32, (1, 16), 1)
    sub8 = lax.broadcasted_iota(jnp.int32, (8, 128), 0)
    mixed = []
    for j in range(2):
        acc = [jnp.zeros((8, 128), F32) for _ in range(8)]
        for i in range(8):
            qd = jnp.broadcast_to(ct[0:64, 8 * j + i : 8 * j + i + 1], (64, 128)) * decb[j * 512 + i * 64 : j * 512 + (i + 1) * 64]
            for k in range(8):
                q8 = qd[8 * k : 8 * k + 8]
                r = i * 64 + 8 * k
                for l in range(8):
                    acc[l] = acc[l] + q8 * st[j, r : r + 8, 128 * l : 128 * l + 128]
        read = jnp.zeros((8, 128), F32)
        for l in range(8):
            read = jnp.where(sub8 == l, jnp.sum(acc[l], axis=0, keepdims=True), read)
        sqk = jnp.sum(jnp.where((lane >= 8 * j) & (lane < 8 * j + 8), dotqk, 0.0), axis=1, keepdims=True)
        read = (read + sqk * val[8 * j : 8 * j + 8]) * (512 ** -0.5)
        tot = jnp.sum(jnp.sum(read * read, axis=1, keepdims=True), axis=0, keepdims=True)
        nrm = lax.rsqrt(tot * (1.0 / 1024) + EPS)
        g = gat[8 * j : 8 * j + 8]
        mixed.append(read * nrm * hg[...].astype(F32) * (g / (1.0 + jnp.exp(-g))))
    mixed = jnp.concatenate(mixed, axis=0).astype(BF16)
    mx[...] = mixed
    mb[z] = mixed
    for o in far:
        remote(mx, mb.at[z], ssem.at[2], r3.at[z], 2 * chip(o) + c).start()

    for j in range(2):
        for i in range(8):
            kc = jnp.broadcast_to(ct[64:128, 8 * j + i : 8 * j + i + 1], (64, 128))
            for k in range(8):
                r = i * 64 + 8 * k
                d8 = decb[j * 512 + r : j * 512 + r + 8]
                k8 = kc[8 * k : 8 * k + 8]
                for l in range(8):
                    sl = (j, slice(r, r + 8), slice(128 * l, 128 * l + 128))
                    st[sl] = st[sl] * d8 + k8 * val[8 * j + l : 8 * j + l + 1]
    cps[15].wait()
    wref = wo.at[:, pl.ds(lother, 128)]
    remote(wref, wref, rsem.at[3], rsem.at[3], me).wait_recv()
    for o in near:
        zz = chip(o)
        blk = mb.at[zz]
        remote(blk, blk, r3.at[zz], r3.at[zz], me).wait_recv()
    PITCH = 17
    for s in range(T):
        ff[s * PITCH : s * PITCH + 16] = mb[s].astype(F32)
    lhs = []
    for kb in range(N // 2):
        lhs.append(ff[pl.ds(kb, T, stride=PITCH), :].astype(BF16))
    part = mm(jnp.concatenate(lhs, axis=1), wo[...]).astype(BF16)

    sb[...] = mm(ch[...], part).reshape(N, 2, 256).astype(BF16)
    for o in far:
        for cc in (0, 1):
            j = 2 * chip(o) + cc
            remote(sb.at[j], eb.at[me], ssem.at[3], r4.at[z], j).start()
    remote(sb.at[other], eb.at[me], ssem.at[3], r4.at[z], other).start()
    eb[me] = sb[me]
    ps[0] = part[:, :128]
    ps[1] = part[:, 128:]
    remote(ps.at[1 - c], pr, ssem.at[6], rsem.at[2], other).start()
    for cp in cps[16:18]:
        cp.wait()
    ssq = jnp.zeros((2, 256), F32)
    ga = jnp.zeros((2, 512), F32)
    up = jnp.zeros((2, 512), F32)
    pairs = [[0]] + [[d, -d] for d in range(1, C // 2)] + [[C // 2]]
    for group in pairs:
        zs = [arrived(eb, r4, o) for o in group]
        for zz in zs:
            branch = (eb[2 * zz].astype(F32) + eb[2 * zz + 1].astype(F32)).astype(BF16).astype(F32)
            x = (rs[zz, 0:2] + branch).astype(BF16).astype(F32)
            gain = jnp.concatenate([g2f[pl.ds(2 * zz, 1)], g2f[pl.ds(2 * zz + 1, 1)]], axis=1)
            ssq = ssq + x * x
            y = (x * gain).astype(BF16)
            at = pl.multiple_of(zz * 256, 256)
            ga = ga + mm(y, eg[pl.ds(at, 256), :])
            up = up + mm(y, eu[pl.ds(at, 256), :])
    scale = lax.rsqrt(jnp.sum(ssq, axis=1, keepdims=True) * (1.0 / (128 * N)) + EPS)
    ga = ga * scale
    act = (ga / (1.0 + jnp.exp(-ga)) * (up * scale) * rw[0:2]).astype(BF16)

    cps[18].wait()
    for group in pairs[::-1]:
        zs = [chip(o) for o in group]
        rows = [mm(act, ed[:, pl.ds(pl.multiple_of(zz * 256, 256), 256)]).astype(BF16) for zz in zs]
        for zz, both in zip(zs, rows):
            for cc in (0, 1):
                db[2 * zz + cc] = both[:, 128 * cc : 128 * cc + 128]
                if group[0]:
                    remote(db.at[2 * zz + cc], rb.at[me], ssem.at[4], rsem.at[1], 2 * zz + cc).start()
    remote(db.at[2 * z + 1 - c], rb.at[me], ssem.at[4], rsem.at[1], 2 * z + 1 - c).start()
    rb[me] = db[me]
    remote(pr, pr, rsem.at[2], rsem.at[2], me).wait_recv()
    branch = (ps[c].astype(F32) + pr[...].astype(F32)).astype(BF16).astype(F32)
    stream = (res[...].astype(F32) + branch).astype(BF16).astype(F32)
    ref = rb.at[pl.ds(0, N - 1)]
    remote(ref, ref, rsem.at[1], rsem.at[1], me).wait_recv()
    back = mm(cht[...], rb[...].reshape(2 * N, 128))
    out_ref[...] = (stream + back).astype(BF16)

    for stage, ref in ((0, xb.at[pl.ds(0, N - 1)]), (2, mb.at[pl.ds(0, C - 1)]), (6, pr), (3, eb.at[pl.ds(0, N - 1)]), (4, rb.at[pl.ds(0, N - 1)])):
        remote(ref, ref, ssem.at[stage], ssem.at[stage], me).wait_send()
    wsend.wait_send()

    @pl.when(core == c)
    def _():
        ref = rq.at[pl.ds(0, S - 1)]
        remote(ref, ref, ssem.at[1], ssem.at[1], me).wait_send()

    @pl.when(core != c)
    def _():
        remote(rq, rq, ssem.at[1], ssem.at[1], me).wait_send()


def per_device(N, residual, head_states, first_gain, w_query, w_key, w_value, w_gate, w_low, w_decay, decay_bias,
               head_gain, w_output, second_gain, routes, group_logits, expert_logits, expert_gate, expert_up, expert_down):
    args = (
        residual, head_states, first_gain.reshape(-1, 128), w_query.T, w_key.T, w_value, w_gate, w_low.T, w_decay,
        decay_bias.reshape(-1, 128), head_gain.reshape(-1, 128), w_output, second_gain.reshape(-1, 128),
        routes.T, group_logits.T, expert_logits.T, expert_gate, expert_up, expert_down,
    )
    V = pltpu.VMEM
    args = tuple(pltpu.with_memory_space_constraint(a, pltpu.HBM) for a in args)
    D = 128 * N
    SB = BF16
    scratch = [
        V((16, 128), BF16), V((N, 128), BF16), V((144, D), BF16), V((D, 256), BF16),
        V((16, 1024), BF16), V((8, 128), F32), V((8, 128), BF16), V((D // 2, 256), BF16), V((N, 128), BF16),
        V((2, 16), jnp.int32), V((4, 16), F32), V((2, 16), F32), V((D, 512), BF16), V((D, 512), BF16), V((512, D), BF16),
        V((N, 128), F32), V((N, 128), F32), V((N, 16, 128), BF16), V((16, 4, 128), F32), V((16, 4, 128), F32),
        V((1024, 128), F32), V((128, 128), F32), V((16, 128), BF16), V((N // 2, 16, 128), BF16), V((17 * 16, 128), F32),
        V((2 * N, 16), BF16), V((16, 2 * N), BF16), V((N, 2, 256), SB), V((N, 2, 256), SB), V((N, 2, 128), SB), V((N, 2, 128), SB), V((N // 2, 8, 256), F32), V((2, 16, 128), BF16), V((16, 128), BF16),
        pltpu.SemaphoreType.DMA((19,)), pltpu.SemaphoreType.DMA((7,)), pltpu.SemaphoreType.DMA((4,)),
        pltpu.SemaphoreType.DMA((N // 2,)), pltpu.SemaphoreType.DMA((N // 2,)), pltpu.SemaphoreType.DMA((N // 2,)),
        pltpu.SemaphoreType.DMA((1,)),
    ]
    lo, ns = pl.pallas_call(
        functools.partial(kernel, N),
        out_shape=(jax.ShapeDtypeStruct(residual.shape, BF16), jax.ShapeDtypeStruct(head_states.shape, F32)),
        in_specs=[pl.BlockSpec(memory_space=pl.ANY)] * len(args),
        out_specs=(pl.BlockSpec(memory_space=pltpu.VMEM), pl.BlockSpec(memory_space=pltpu.VMEM)),
        scratch_shapes=scratch,
        compiler_params=pltpu.CompilerParams(collective_id=0, has_side_effects=True, vmem_limit_bytes=40 * 1024 * 1024),
    )(*args)

    def tail(lo_ref, ns_ref, o_ref, on_ref, sem):
        cps = [pltpu.make_async_copy(lo_ref, o_ref, sem.at[8])]
        for i in range(8):
            at = (i // 4, pl.ds(128 * (i % 4), 128))
            cps.append(pltpu.make_async_copy(ns_ref.at[at], on_ref.at[at], sem.at[i]))
        for cp in cps:
            cp.start()
        for cp in cps:
            cp.wait()

    return pl.pallas_call(
        tail,
        out_shape=(jax.ShapeDtypeStruct(residual.shape, BF16), jax.ShapeDtypeStruct(head_states.shape, F32)),
        in_specs=[pl.BlockSpec(memory_space=pltpu.VMEM), pl.BlockSpec(memory_space=pltpu.VMEM)],
        out_specs=(pl.BlockSpec(memory_space=pl.ANY), pl.BlockSpec(memory_space=pl.ANY)),
        scratch_shapes=[pltpu.SemaphoreType.DMA((9,))],
        compiler_params=pltpu.CompilerParams(vmem_limit_bytes=16 * 1024 * 1024),
    )(lo, ns)


def solution(mesh):
    N = mesh.shape["ep"]
    return jax.shard_map(
        functools.partial(per_device, N),
        mesh=mesh,
        in_specs=(
            P("grp", "ep"), P(("grp", "ep"), None, None), P(), P(None, "ep"), P(None, "ep"), P(None, "ep"), P(None, "ep"),
            P(), P(), P(), P(), P(None, "ep"), P(), P("grp", None), P("grp", None), P("grp", None),
            P("ep", None, None), P("ep", None, None), P("ep", None, None),
        ),
        out_specs=(P("grp", "ep"), P(("grp", "ep"), None, None)),
        check_vma=False,
    )
```

```python
import functools
import jax
import jax.numpy as jnp
from jax import lax
from jax.experimental import pallas as pl
from jax.experimental.pallas import tpu as pltpu
from jax.sharding import PartitionSpec as P

HEADS = 4
GROUPS = 4
TOP = 2
EPS = 1e-6
TAU = 16.0
MESH = pl.DeviceIdType.MESH
BF16 = jnp.bfloat16
F32 = jnp.float32
NT = (((1,), (1,)), ((), ()))
NN = (((1,), (0,)), ((), ()))
TN = (((0,), (0,)), ((), ()))


def mm(a, b, dims=NN, precision=None):
    return lax.dot_general(a, b, dims, precision=precision, preferred_element_type=F32)


def kernel(
    N,
    res_h, st_h, g1_h, wq_h, wk_h, wv_h, wg_h, wl_h, wd_h, bias_h, hg_h, wo_h, g2_h,
    rt_h, gl_h, el_h, eg_h, eu_h, ed_h,
    out_ref, st,
    res, g1, wqk, wvg, wd, bias, hg, wo, g2, rt, gl, el, eg, eu, ed,
    g1f, g2f, xb, pj, rq, decb, mx, mb, ff, ch, cht, sb, eb, db, rb, rs, ps, pr,
    lsem, ssem, rsem, r1, r3, r4, r2,
):
    me = lax.axis_index("ep")
    C = N // 2
    z, c = me // 2, lax.rem(me, 2)
    T = res.shape[0]
    far = [C // 2] + [s * d for d in range(C // 2 - 1, 0, -1) for s in (1, -1)]
    near = far[::-1]

    def chip(o):
        return lax.rem(z + (o + C), C)

    barrier = pltpu.get_barrier_semaphore()
    reach = C // 4
    close = [o for o in near if abs(o) <= reach]
    for o in close[::-1]:
        for cc in (0, 1):
            pl.semaphore_signal(barrier, inc=1, device_id={"ep": 2 * chip(o) + cc}, device_id_type=MESH)
    pl.semaphore_signal(barrier, inc=1, device_id={"ep": 2 * z + 1 - c}, device_id_type=MESH)

    half = pl.multiple_of(c * 1024, 1024)
    hrow = pl.multiple_of(c * 8, 8)
    kmine, kother = pl.multiple_of(c * 2048, 2048), pl.multiple_of(2048 - c * 2048, 2048)
    lmine, lother = pl.multiple_of(c * 128, 128), pl.multiple_of(128 - c * 128, 128)
    loads = [
        (res_h, res), (g1_h, g1), (g2_h, g2), (hg_h, hg), (rt_h, rt), (gl_h, gl), (el_h, el),
        (bias_h.at[pl.ds(hrow, 8)], bias), (wd_h.at[:, pl.ds(half, 1024)], wd),
        (wq_h, wqk.at[pl.ds(0, 64)]), (wk_h, wqk.at[pl.ds(64, 64)]), (wl_h, wqk.at[pl.ds(128, 16)]),
        (wv_h, wvg.at[:, pl.ds(0, 128)]), (wg_h, wvg.at[:, pl.ds(128, 128)]),
        (st_h, st), (wo_h.at[pl.ds(kmine, 2048)], wo.at[:, pl.ds(lmine, 128)]), (eg_h.at[0], eg), (eu_h.at[0], eu), (ed_h.at[0], ed),
    ]
    cps = [pltpu.make_async_copy(s, d, lsem.at[i]) for i, (s, d) in enumerate(loads)]
    for cp in cps[:14]:
        cp.start()
    cps[0].wait()

    xb[me] = res[...]
    pl.semaphore_wait(barrier, 2 * len(close) + 1)

    def remote(src, dst, send, recv, j):
        return pltpu.make_async_remote_copy(
            src_ref=src, dst_ref=dst, send_sem=send, recv_sem=recv, device_id={"ep": j}, device_id_type=MESH
        )


    def arrived(buf, sem, o):
        zz = chip(o)
        ref = buf.at[pl.ds(2 * zz, 2)] if o else buf.at[2 * zz]
        remote(ref, ref, sem.at[zz], sem.at[zz], me).wait_recv()
        return zz

    for o in close[::-1]:
        for cc in (0, 1):
            remote(res, xb.at[me], ssem.at[0], r1.at[z], 2 * chip(o) + cc).start()
    remote(res, xb.at[me], ssem.at[0], r1.at[z], 2 * z + 1 - c).start()
    for cp in cps[1:9]:
        cp.wait()
    g1f[...] = g1[...].astype(F32)
    g2f[...] = g2[...].astype(F32)

    routes = rt[...]
    gexp = jnp.exp(gl[...])
    gprob = gexp / jnp.sum(gexp, axis=0, keepdims=True)
    per_group = N // GROUPS
    grow = lax.broadcasted_iota(jnp.int32, gprob.shape, 0)
    lo = grow * per_group
    first = jnp.broadcast_to(routes[0:1], gprob.shape)
    inside = (first >= lo) & (first < lo + per_group)
    gpick = jnp.sum(jnp.where(inside, gprob, 0.0), axis=0, keepdims=True)
    eexp = jnp.exp(el[...])
    weight = eexp / jnp.sum(eexp, axis=0, keepdims=True) * gpick
    before = (
        lax.broadcasted_iota(jnp.int32, (T, T), 0) < lax.broadcasted_iota(jnp.int32, (T, T), 1)
    ).astype(BF16)
    slots_all = 2 * N
    row = lax.broadcasted_iota(jnp.int32, (slots_all, T), 0)
    expert = lax.shift_right_logical(row, 1)
    r0 = jnp.broadcast_to(routes[0:1], (slots_all, T))
    r1_ = jnp.broadcast_to(routes[1:2], (slots_all, T))
    hit = jnp.where((r0 == expert) | (r1_ == expert), 1.0, 0.0)
    slot = mm(hit.astype(BF16), before)
    parity = (row - 2 * expert).astype(F32)
    chv = jnp.where(slot == parity, hit, 0.0)
    ch[...] = chv.astype(BF16)
    cht[...] = chv.T.astype(BF16)
    my_hit = jnp.where(routes == me, 1.0, 0.0)
    share = jnp.sum(weight * my_hit, axis=0, keepdims=True)
    mine = jnp.sum(my_hit, axis=0, keepdims=True)
    my_slot = mm(jnp.broadcast_to(mine, (8, T)).astype(BF16), before)
    srow = lax.broadcasted_iota(jnp.int32, (8, T), 0).astype(F32)
    rw = jnp.sum(jnp.where(my_slot == srow, jnp.broadcast_to(mine * share, (8, T)), 0.0), axis=1, keepdims=True)
    my_rows = jnp.where(my_slot == srow, jnp.broadcast_to(mine, (8, T)), 0.0).astype(BF16)

    for o in close + [0]:
        zz = arrived(xb, r1, o)
        if 0 < o <= reach or -reach < o < 0:
            to = chip(-reach if o > 0 else reach)
            for cc in (0, 1):
                blk = xb.at[2 * zz + c]
                remote(blk, blk, ssem.at[0], r1.at[zz], 2 * to + cc).start()
    for cp in cps[14:]:
        cp.start()
    for cp in cps[9:14]:
        cp.wait()
    ssq = jnp.zeros((T, 256), F32)
    vg = jnp.zeros((T, 256), F32)
    qk = jnp.zeros((T, 144), F32)
    for o in [0] + near:
        zz = chip(o) if abs(o) <= reach else arrived(xb, r1, o)
        x = jnp.concatenate([xb[2 * zz], xb[2 * zz + 1]], axis=1).astype(F32)
        gain = jnp.concatenate([g1f[pl.ds(2 * zz, 1)], g1f[pl.ds(2 * zz + 1, 1)]], axis=1)
        ssq = ssq + x * x
        y = (x * gain).astype(BF16)
        at = pl.multiple_of(zz * 256, 256)
        vg = vg + mm(y, wvg[pl.ds(at, 256), :])
        qk = qk + mm(y, wqk[:, pl.ds(at, 256)], NT)
    scale = lax.rsqrt(jnp.sum(ssq, axis=1, keepdims=True) * (1.0 / (128 * N)) + EPS)
    vg = (vg * scale).astype(BF16).astype(F32)
    low = qk[:, 128:144] * scale
    qk = (qk[:, :128] * scale).astype(BF16).astype(F32)

    for s in range(T):
        pj[s, 0:1] = vg[s : s + 1, :128]
        pj[s, 1:2] = vg[s : s + 1, 128:]
        pj[s, 2:3] = qk[s : s + 1]
    S = N // 2
    core = me // S
    mine_at = lax.rem(me, S)
    for o in far:
        s = chip(o)
        remote(pj.at[s], rq.at[mine_at], ssem.at[1], r2.at[mine_at // 8], 2 * s + core).start()

    @pl.when(core != c)
    def _():
        remote(pj.at[z], rq.at[mine_at], ssem.at[1], r2.at[mine_at // 8], 2 * z + core).start()

    @pl.when(core == c)
    def _():
        rq[mine_at] = pj[z]

    other = 2 * z + 1 - c
    wsend = remote(wo_h.at[pl.ds(kother, 2048)], wo.at[:, pl.ds(lmine, 128)], ssem.at[5], rsem.at[3], other)
    wsend.start()
    for s in range(C):
        both = jnp.concatenate([xb[2 * s], xb[2 * s + 1]], axis=1)
        rs[s] = mm(my_rows, both)

    pick = jnp.where(lax.broadcasted_iota(jnp.int32, (T, 128), 0) == z, 1.0, 0.0)
    lowcol = mm(low, pick, TN, lax.Precision.HIGHEST)
    pre = mm(wd[...].astype(F32), lowcol, TN, lax.Precision.HIGHEST)
    bcol = bias[...].T
    for b in range(8):
        v = pre[b * 128 : (b + 1) * 128] + bcol[:, b : b + 1]
        ls = jnp.minimum(v, 0.0) - jnp.log(1.0 + jnp.exp(-jnp.abs(v)))
        decb[b // 4, (b % 4) * 128 : (b % 4 + 1) * 128] = jnp.exp(ls * (1.0 / TAU))
    cps[14].wait()

    sub8 = lax.broadcasted_iota(jnp.int32, (8, 128), 0)
    quarter = C // 4
    first = lax.rem((lax.rem(z - c * (C // 2) + C, C) + quarter) // (2 * quarter), 2)
    heads = []
    for j in (first, 1 - first):
        own = jnp.logical_and(core == c, mine_at // 8 == j)

        @pl.when(own)
        def _():
            ref = rq.at[pl.ds(0, 7)]
            remote(ref, ref, r2.at[j], r2.at[j], me).wait_recv()

        @pl.when(jnp.logical_not(own))
        def _():
            ref = rq.at[pl.ds(0, 8)]
            remote(ref, ref, r2.at[j], r2.at[j], me).wait_recv()

        allv = rq[pl.ds(pl.multiple_of(8 * j, 8), 8)]
        val = allv[:, 0, :]
        g = allv[:, 1, :]
        ct = allv[:, 2, :].T
        heads.append((j, val, ct))
        sqk = jnp.sum(jnp.sum(ct[0:64] * ct[64:128], axis=0, keepdims=True), axis=1, keepdims=True)
        acc = [jnp.zeros((8, 128), F32) for _ in range(8)]
        for i in range(8):
            qd = jnp.broadcast_to(ct[0:64, i : i + 1], (64, 128)) * decb[j, i * 64 : (i + 1) * 64]
            for k in range(8):
                q8 = qd[8 * k : 8 * k + 8]
                r = i * 64 + 8 * k
                for l in range(8):
                    acc[l] = acc[l] + q8 * st[j, r : r + 8, 128 * l : 128 * l + 128]
        read = jnp.zeros((8, 128), F32)
        for l in range(8):
            read = jnp.where(sub8 == l, jnp.sum(acc[l], axis=0, keepdims=True), read)
        read = (read + sqk * val) * (512 ** -0.5)
        tot = jnp.sum(jnp.sum(read * read, axis=1, keepdims=True), axis=0, keepdims=True)
        nrm = lax.rsqrt(tot * (1.0 / 1024) + EPS)
        mixed = (read * nrm * hg[...].astype(F32) * (g / (1.0 + jnp.exp(-g)))).astype(BF16)
        mx[j] = mixed
        mb[z, j] = mixed
    for o in far:
        remote(mx, mb.at[z], ssem.at[2], r3.at[z], 2 * chip(o) + c).start()

    for j, val, ct in heads:
        for i in range(8):
            kc = jnp.broadcast_to(ct[64:128, i : i + 1], (64, 128))
            for k in range(8):
                r = i * 64 + 8 * k
                d8 = decb[j, r : r + 8]
                k8 = kc[8 * k : 8 * k + 8]
                for l in range(8):
                    sl = (j, slice(r, r + 8), slice(128 * l, 128 * l + 128))
                    st[sl] = st[sl] * d8 + k8 * val[l : l + 1]
    cps[15].wait()
    wref = wo.at[:, pl.ds(lother, 128)]
    remote(wref, wref, rsem.at[3], rsem.at[3], me).wait_recv()
    for o in near:
        zz = chip(o)
        blk = mb.at[zz]
        remote(blk, blk, r3.at[zz], r3.at[zz], me).wait_recv()
    PITCH = 17
    for s in range(T):
        ff[s * PITCH : s * PITCH + 16] = jnp.concatenate([mb[s, 0].astype(F32), mb[s, 1].astype(F32)], axis=0)
    lhs = []
    for kb in range(N // 2):
        lhs.append(ff[pl.ds(kb, T, stride=PITCH), :].astype(BF16))
    part = mm(jnp.concatenate(lhs, axis=1), wo[...]).astype(BF16)

    sb[...] = mm(ch[...], part).reshape(N, 2, 256).astype(BF16)
    for o in far:
        for cc in (0, 1):
            j = 2 * chip(o) + cc
            remote(sb.at[j], eb.at[me], ssem.at[3], r4.at[z], j).start()
    remote(sb.at[other], eb.at[me], ssem.at[3], r4.at[z], other).start()
    eb[me] = sb[me]
    ps[0] = part[:, :128]
    ps[1] = part[:, 128:]
    remote(ps.at[1 - c], pr, ssem.at[6], rsem.at[2], other).start()
    for cp in cps[16:18]:
        cp.wait()
    ssq = jnp.zeros((2, 256), F32)
    ga = jnp.zeros((2, 512), F32)
    up = jnp.zeros((2, 512), F32)
    pairs = [[0]] + [[d, -d] for d in range(1, C // 2)] + [[C // 2]]
    for group in pairs:
        zs = [arrived(eb, r4, o) for o in group]
        for zz in zs:
            branch = (eb[2 * zz].astype(F32) + eb[2 * zz + 1].astype(F32)).astype(BF16).astype(F32)
            x = (rs[zz, 0:2] + branch).astype(BF16).astype(F32)
            gain = jnp.concatenate([g2f[pl.ds(2 * zz, 1)], g2f[pl.ds(2 * zz + 1, 1)]], axis=1)
            ssq = ssq + x * x
            y = (x * gain).astype(BF16)
            at = pl.multiple_of(zz * 256, 256)
            ga = ga + mm(y, eg[pl.ds(at, 256), :])
            up = up + mm(y, eu[pl.ds(at, 256), :])
    scale = lax.rsqrt(jnp.sum(ssq, axis=1, keepdims=True) * (1.0 / (128 * N)) + EPS)
    ga = ga * scale
    act = (ga / (1.0 + jnp.exp(-ga)) * (up * scale) * rw[0:2]).astype(BF16)

    cps[18].wait()
    for group in pairs[::-1]:
        zs = [chip(o) for o in group]
        rows = [mm(act, ed[:, pl.ds(pl.multiple_of(zz * 256, 256), 256)]).astype(BF16) for zz in zs]
        for zz, both in zip(zs, rows):
            for cc in (0, 1):
                db[2 * zz + cc] = both[:, 128 * cc : 128 * cc + 128]
                if group[0]:
                    remote(db.at[2 * zz + cc], rb.at[me], ssem.at[4], rsem.at[1], 2 * zz + cc).start()
    remote(db.at[2 * z + 1 - c], rb.at[me], ssem.at[4], rsem.at[1], 2 * z + 1 - c).start()
    rb[me] = db[me]
    remote(pr, pr, rsem.at[2], rsem.at[2], me).wait_recv()
    branch = (ps[c].astype(F32) + pr[...].astype(F32)).astype(BF16).astype(F32)
    stream = (res[...].astype(F32) + branch).astype(BF16).astype(F32)
    ref = rb.at[pl.ds(0, N - 1)]
    remote(ref, ref, rsem.at[1], rsem.at[1], me).wait_recv()
    back = mm(cht[...], rb[...].reshape(2 * N, 128))
    out_ref[...] = (stream + back).astype(BF16)

    for stage, ref in ((0, xb.at[pl.ds(0, N - 1)]), (2, mb.at[pl.ds(0, C - 1)]), (6, pr), (3, eb.at[pl.ds(0, N - 1)]), (4, rb.at[pl.ds(0, N - 1)])):
        remote(ref, ref, ssem.at[stage], ssem.at[stage], me).wait_send()
    wsend.wait_send()

    @pl.when(core == c)
    def _():
        ref = rq.at[pl.ds(0, S - 1)]
        remote(ref, ref, ssem.at[1], ssem.at[1], me).wait_send()

    @pl.when(core != c)
    def _():
        remote(rq, rq, ssem.at[1], ssem.at[1], me).wait_send()


def per_device(N, residual, head_states, first_gain, w_query, w_key, w_value, w_gate, w_low, w_decay, decay_bias,
               head_gain, w_output, second_gain, routes, group_logits, expert_logits, expert_gate, expert_up, expert_down):
    args = (
        residual, head_states, first_gain.reshape(-1, 128), w_query.T, w_key.T, w_value, w_gate, w_low.T, w_decay,
        decay_bias.reshape(-1, 128), head_gain.reshape(-1, 128), w_output, second_gain.reshape(-1, 128),
        routes.T, group_logits.T, expert_logits.T, expert_gate, expert_up, expert_down,
    )
    V = pltpu.VMEM
    args = tuple(pltpu.with_memory_space_constraint(a, pltpu.HBM) for a in args)
    D = 128 * N
    SB = BF16
    scratch = [
        V((16, 128), BF16), V((N, 128), BF16), V((144, D), BF16), V((D, 256), BF16),
        V((16, 1024), BF16), V((8, 128), F32), V((8, 128), BF16), V((D // 2, 256), BF16), V((N, 128), BF16),
        V((2, 16), jnp.int32), V((4, 16), F32), V((2, 16), F32), V((D, 512), BF16), V((D, 512), BF16), V((512, D), BF16),
        V((N, 128), F32), V((N, 128), F32), V((N, 16, 128), BF16), V((16, 4, 128), F32), V((16, 4, 128), F32),
        V((2, 512, 128), F32), V((2, 8, 128), BF16), V((N // 2, 2, 8, 128), BF16), V((17 * 16, 128), F32),
        V((2 * N, 16), BF16), V((16, 2 * N), BF16), V((N, 2, 256), SB), V((N, 2, 256), SB), V((N, 2, 128), SB), V((N, 2, 128), SB), V((N // 2, 8, 256), F32), V((2, 16, 128), BF16), V((16, 128), BF16),
        pltpu.SemaphoreType.DMA((19,)), pltpu.SemaphoreType.DMA((7,)), pltpu.SemaphoreType.DMA((4,)),
        pltpu.SemaphoreType.DMA((N // 2,)), pltpu.SemaphoreType.DMA((N // 2,)), pltpu.SemaphoreType.DMA((N // 2,)),
        pltpu.SemaphoreType.DMA((2,)),
    ]
    lo, ns = pl.pallas_call(
        functools.partial(kernel, N),
        out_shape=(jax.ShapeDtypeStruct(residual.shape, BF16), jax.ShapeDtypeStruct(head_states.shape, F32)),
        in_specs=[pl.BlockSpec(memory_space=pl.ANY)] * len(args),
        out_specs=(pl.BlockSpec(memory_space=pltpu.VMEM), pl.BlockSpec(memory_space=pltpu.VMEM)),
        scratch_shapes=scratch,
        compiler_params=pltpu.CompilerParams(collective_id=0, has_side_effects=True, vmem_limit_bytes=40 * 1024 * 1024),
    )(*args)

    def tail(lo_ref, ns_ref, o_ref, on_ref, sem):
        cps = [pltpu.make_async_copy(lo_ref, o_ref, sem.at[8])]
        for i in range(8):
            at = (i // 4, pl.ds(128 * (i % 4), 128))
            cps.append(pltpu.make_async_copy(ns_ref.at[at], on_ref.at[at], sem.at[i]))
        for cp in cps:
            cp.start()
        for cp in cps:
            cp.wait()

    return pl.pallas_call(
        tail,
        out_shape=(jax.ShapeDtypeStruct(residual.shape, BF16), jax.ShapeDtypeStruct(head_states.shape, F32)),
        in_specs=[pl.BlockSpec(memory_space=pltpu.VMEM), pl.BlockSpec(memory_space=pltpu.VMEM)],
        out_specs=(pl.BlockSpec(memory_space=pl.ANY), pl.BlockSpec(memory_space=pl.ANY)),
        scratch_shapes=[pltpu.SemaphoreType.DMA((9,))],
        compiler_params=pltpu.CompilerParams(vmem_limit_bytes=16 * 1024 * 1024),
    )(lo, ns)


def solution(mesh):
    N = mesh.shape["ep"]
    return jax.shard_map(
        functools.partial(per_device, N),
        mesh=mesh,
        in_specs=(
            P("grp", "ep"), P(("grp", "ep"), None, None), P(), P(None, "ep"), P(None, "ep"), P(None, "ep"), P(None, "ep"),
            P(), P(), P(), P(), P(None, "ep"), P(), P("grp", None), P("grp", None), P("grp", None),
            P("ep", None, None), P("ep", None, None), P("ep", None, None),
        ),
        out_specs=(P("grp", "ep"), P(("grp", "ep"), None, None)),
        check_vma=False,
    )
```
